32 devices in a mesh: sp: 16 (over z, y, x), tp: 2 (over core).
Axes of the slice: x: 2, y: 2, z: 4, core: 2. Of those that a mesh axis runs over, the one named last changes fastest.
Arguments:
- tokens: bfloat16 [4096, 2048], P('sp', 'tp'), may hold values from -24 to 24
- value_weight: bfloat16 [2, 2048, 2048], P(None, 'sp', 'tp'), may hold values from -0.125 to 0.125
- outer_weight: bfloat16 [2, 2048, 2048], P(None, 'sp', 'tp'), may hold values from -0.125 to 0.125
- inner_weight: bfloat16 [2, 2048, 2048], P(None, 'sp', 'tp'), may hold values from -0.125 to 0.125
- conv_taps: float32 [2, 3, 2048], P(None, None, 'tp'), may hold values from -3.5 to 3.5
- output_weight: bfloat16 [2, 2048, 2048], P(None, 'tp', 'sp'), may hold values from -2 to 2
- norm_gain: float32 [2, 2048], P(None, 'tp'), may hold values from 0.1 to 1.9
- norm_bias: float32 [2, 2048], P(None, 'tp'), may hold values from -3 to 3
Outputs:
- mixed_out: bfloat16 [4096, 2048], P('sp', 'tp')
The draws below stay inside these ranges and needn't reach their ends.
All inputs are finite; a program needn't handle non-finite values.
Results may differ from the reference program's by a relative error of at most 0.03.
Values may be sent and summed in bfloat16 or wider, within the bound.
A program may use at most 64 MiB of HBM per device.

```python
import jax
import jax.numpy as jnp
from jax import lax

D = 2048
CW = 2048
CONV_K = 3
LAYERS = 2
TOKENS = 4096
N_TP = 2


def column_scale(key, width):
    position = jnp.arange(width, dtype=jnp.float32) / width
    rough = jax.random.uniform(key, (width,), jnp.float32, 0.6, 1.4)
    return jnp.exp(jnp.log(4.0) * position) * rough


def draw_tokens(key, part):
    first, second = jax.random.split(jax.random.fold_in(key, 11), 2)
    scales = column_scale(second, D)
    base = jnp.clip(jax.random.normal(first, (TOKENS, D), jnp.float32), -5.0, 5.0)
    return jnp.clip(base * scales[None, :], -24.0, 24.0).astype(jnp.bfloat16)


def draw_output_weight(key, part):
    first, second = jax.random.split(jax.random.fold_in(key, 23), 2)
    scales = column_scale(second, D)
    base = jnp.clip(jax.random.normal(first, (LAYERS, CW, D), jnp.float32), -5.0, 5.0)
    values = base * scales[None, None, :] * CW ** (-0.5)
    return jnp.clip(values, -2.0, 2.0).astype(jnp.bfloat16)


def block_levels(rng, shape, pieces, low, top_value):
    loudness, own = 1.0, jax.random.fold_in(rng, 6)
    for dim, shards_of in pieces:
        draws = jnp.exp(jax.random.uniform(jax.random.fold_in(own, dim), (shards_of,), jnp.float32, low / len(pieces), top_value / len(pieces)))
        loudness = loudness * jnp.repeat(draws, shape[dim] // shards_of).reshape([-1 if axis == dim else 1 for axis in range(len(shape))])
    return loudness


def scatter_about(own_key, extent, spread, reach, cuts=(), kind=jnp.bfloat16):
    level = block_levels(own_key, extent, cuts, -0.22, 0.18) if cuts else 1.0
    array = jax.random.normal(own_key, extent, jnp.float32) * spread * level
    return jnp.minimum(jnp.maximum(array, -reach), reach).astype(kind)


def setup_inputs(seed: int = 0) -> dict:
    key_list = jax.random.split(jax.random.key(seed), 9)
    return {
        "tokens": draw_tokens(jax.random.fold_in(key_list[8], 71), 0),
        "value_weight": scatter_about(key_list[1], (LAYERS, D, CW), D ** -0.5, 0.125, ((1, 16), (2, 2))),
        "outer_weight": scatter_about(key_list[2], (LAYERS, D, CW), D ** -0.5, 0.125, ((1, 16), (2, 2))),
        "inner_weight": scatter_about(key_list[3], (LAYERS, D, CW), D ** -0.5, 0.125, ((1, 16), (2, 2))),
        "conv_taps": scatter_about(key_list[4], (LAYERS, CONV_K, CW), CONV_K ** -0.5, 3.5, ((2, 2),), jnp.float32),
        "output_weight": draw_output_weight(jax.random.fold_in(key_list[8], 71), 0),
        "norm_gain": jnp.clip(1.0 + 0.18 * jax.random.normal(key_list[6], (LAYERS, D), jnp.float32), 0.1, 1.9),
        "norm_bias": scatter_about(key_list[7], (LAYERS, D), 0.5, 3.0, ((1, 2),), jnp.float32),
    }


def reference(tokens, value_weight, outer_weight, inner_weight, conv_taps, output_weight, norm_gain, norm_bias):
    alpha = (2.0 * LAYERS) ** 0.25
    state = tokens
    width = CW // N_TP
    for layer in range(LAYERS):
        u_part = jnp.dot(state, value_weight[layer], preferred_element_type=jnp.float32).astype(jnp.bfloat16)
        outer = jnp.dot(state, outer_weight[layer], preferred_element_type=jnp.float32).astype(jnp.bfloat16)
        inner = jnp.dot(state, inner_weight[layer], preferred_element_type=jnp.float32).astype(jnp.bfloat16)
        gated_in = inner.astype(jnp.float32) * u_part.astype(jnp.float32)
        padded = jnp.concatenate([jnp.zeros((CONV_K - 1, CW), jnp.float32), gated_in], axis=0)
        conv = jnp.zeros_like(gated_in)
        for tap in range(CONV_K):
            conv = conv + conv_taps[layer, tap][None, :] * padded[tap:tap + gated_in.shape[0]]
        gated = (outer.astype(jnp.float32) * conv).astype(jnp.bfloat16)
        branch = jnp.zeros((gated.shape[0], D), jnp.float32)
        for block in range(N_TP):
            part_sum = jnp.dot(gated[:, block * width:(block + 1) * width], output_weight[layer, block * width:(block + 1) * width], preferred_element_type=jnp.float32).astype(jnp.bfloat16)
            branch = branch + lax.optimization_barrier(part_sum).astype(jnp.float32)
        pre = alpha * state.astype(jnp.float32) + branch
        mean = lax.optimization_barrier(jnp.mean(pre, axis=-1, keepdims=True))
        var = lax.optimization_barrier(jnp.mean(jnp.square(pre - mean), axis=-1, keepdims=True))
        normed = (pre - mean) * lax.rsqrt(var + 1e-05)
        state = (normed * norm_gain[layer][None, :] + norm_bias[layer][None, :]).astype(jnp.bfloat16)
    return state
```

```python
import jax
import jax.numpy as jnp
from jax import lax
from jax.experimental import pallas as pl
from jax.experimental.pallas import tpu as pltpu
from jax.sharding import PartitionSpec as P

LANES = 128
EPS = 1e-5


def flip(j, i):
    if i & 1:
        j = j + 1 - 2 * lax.rem(j, 2)
    if i & 2:
        j = j + 2 - 4 * lax.rem(lax.div(j, 2), 2)
    return j


def plane_size(sp, channels):
    q = 4
    while q > 1 and (sp % q or channels // q < LANES or channels % q):
        q //= 2
    return q


def make_kernel(sp, tp, q, layers, taps_count, rows, feats, depth, width, alpha):
    line = sp // q
    units = layers * 4
    model = feats * tp
    per_half = sp // tp

    def kernel(
        tok, val, outw, inn, taps, prj, gain, bias, res,
        xg, win, wout, state, ubuf, obuf, zpad, gated, part, rec1, snd2, rec2, acc, stat, stat_in, halo,
        a_send, a_recv, a_loc, u_send, u_recv, d_send, d_recv,
        g_send, g_recv, g_loc, t_send, t_recv, p_send, p_recv, r_send, r_recv, s_send, s_recv, h_send, h_recv,
    ):
        me = lax.axis_index("sp")
        c = lax.axis_index("tp")
        l = lax.div(me, q)
        j = lax.rem(me, q)

        def at_sp(other):
            return {"sp": other, "tp": c}

        def at_tp(r):
            return {"sp": me, "tp": lax.rem(c + r, tp)}

        def remote(src, dst, ssem, rsem, dev):
            return pltpu.make_async_remote_copy(
                src_ref=src, dst_ref=dst, send_sem=ssem, recv_sem=rsem,
                device_id=dev, device_id_type=pl.DeviceIdType.MESH,
            )

        def peer(i):
            return l * q + flip(j, i)

        barrier = pltpu.get_barrier_semaphore()

        def greet(dev):
            pl.semaphore_signal(barrier, inc=1, device_id=dev, device_id_type=pl.DeviceIdType.MESH)

        for i in range(1, q):
            greet(at_sp(peer(i)))
        for r in range(1, tp):
            greet(at_tp(r))

        @pl.when(l > 0)
        def _():
            greet(at_sp(me - q))

        @pl.when(l < line - 1)
        def _():
            greet(at_sp(me + q))

        neighbours = (l > 0).astype(jnp.int32) + (l < line - 1).astype(jnp.int32)
        pl.semaphore_wait(barrier, (q - 1) + (tp - 1) + neighbours)

        ORDER = (val, inn, outw, prj)

        def own_piece(k, jd):
            layer, w = divmod(k, 4)
            at = pl.ds(pl.multiple_of(jd * width, width), width)
            if w == 3:
                return prj.at[layer, at, :]
            return ORDER[w].at[layer, :, at]

        def landed(k, s):
            layer, w = divmod(k, 4)
            if w == 3:
                return wout.at[layer, s]
            return win.at[layer, w, pl.ds(pl.multiple_of(s * depth, depth), depth), :]

        def block(k, b):
            layer, w = divmod(k, 4)
            if w == 3:
                return wout.at[layer, pl.ds(b * q, q)]
            return win.at[layer, w, pl.ds(pl.multiple_of(b * (q * depth), q * depth), q * depth), :]

        def a_copy(k, i):
            return remote(own_piece(k, flip(j, i)), landed(k, me), a_send.at[k, i], a_recv.at[k, i], at_sp(peer(i)))

        def a_local(k):
            return pltpu.make_async_copy(own_piece(k, j), landed(k, me), a_loc.at[k])

        def scatter_start(k):
            a_local(k).start()
            for i in range(q - 1, 0, -1):
                a_copy(k, i).start()

        def scatter_wait(k):
            a_local(k).wait()
            for i in range(q - 1, 0, -1):
                a_copy(k, i).wait()

        def up(k, s):
            return remote(block(k, l - s), block(k, l - s), u_send.at[k, s], u_recv.at[k, s], at_sp(me + q))

        def down(k, s):
            return remote(block(k, l + s), block(k, l + s), d_send.at[k, s], d_recv.at[k, s], at_sp(me - q))

        def line_start(k, s):
            @pl.when((l - s >= 0) & (l < line - 1))
            def _():
                up(k, s).start()

            @pl.when((l + s < line) & (l > 0))
            def _():
                down(k, s).start()

        def line_recv(k, s):
            @pl.when(l - 1 - s >= 0)
            def _():
                up(k, s).wait_recv()

            @pl.when(l + 1 + s < line)
            def _():
                down(k, s).wait_recv()

        def line_sent(k, s):
            @pl.when((l - s >= 0) & (l < line - 1))
            def _():
                up(k, s).wait_send()

            @pl.when((l + s < line) & (l > 0))
            def _():
                down(k, s).wait_send()

        def src_of(layer):
            return tok if layer == 0 else state.at[layer - 1]

        def spot(layer, jj):
            return xg.at[layer, c, pl.ds(pl.multiple_of(jj * rows, rows), rows), :]

        def g_copy(layer, i):
            return remote(src_of(layer), spot(layer, j), g_send.at[layer, i], g_recv.at[layer, i], at_sp(peer(i)))

        def g_local(layer):
            return pltpu.make_async_copy(src_of(layer), spot(layer, j), g_loc.at[layer])

        def t_copy(layer, r, i):
            jj = flip(j, i)
            src = src_of(layer) if i == 0 else spot(layer, jj)
            return remote(src, spot(layer, jj), t_send.at[layer, r, i], t_recv.at[layer, r, i], at_tp(r))

        def gather_start(layer):
            g_local(layer).start()
            for i in range(q - 1, 0, -1):
                g_copy(layer, i).start()
            for r in range(1, tp):
                t_copy(layer, r, 0).start()

        def gather_forward(layer):
            for i in range(1, q):
                g_copy(layer, i).wait()
                for r in range(1, tp):
                    t_copy(layer, r, i).start()

        def gather_wait(layer):
            g_local(layer).wait()
            for i in range(q):
                for r in range(1, tp):
                    t_copy(layer, r, i).wait()

        def project(layer, w, store):
            def tile(i, carry):
                at = pl.ds(pl.multiple_of(i * rows, rows), rows)
                total = jnp.zeros((rows, width), jnp.float32)
                for cc in range(tp):
                    total = total + jnp.dot(
                        xg[layer, cc, at, :],
                        win[layer, w, pl.ds(cc * feats, feats), :],
                        preferred_element_type=jnp.float32,
                    )
                store(i, total.astype(jnp.bfloat16))
                return carry

            lax.fori_loop(0, q, tile, 0)

        def put_u(i, v):
            ubuf[pl.ds(pl.multiple_of(i * rows, rows), rows), :] = v

        def put_o(i, v):
            obuf[pl.ds(pl.multiple_of(i * rows, rows), rows), :] = v

        def put_z(i, v):
            at = pl.ds(pl.multiple_of(i * rows, rows), rows)
            zpad[pl.ds(pl.multiple_of(8 + i * rows, 8), rows), :] = v.astype(jnp.float32) * ubuf[at, :].astype(jnp.float32)

        def h_copy(layer):
            return remote(
                halo.at[layer, 0], halo.at[layer, 1], h_send.at[layer], h_recv.at[layer], at_sp(me + q)
            )

        def halo_start(layer):
            halo[layer, 0] = zpad[pl.ds(q * rows, 8), :]

            @pl.when(l < line - 1)
            def _():
                h_copy(layer).start()

        def halo_wait(layer):
            zpad[0:8, :] = jnp.zeros((8, width), jnp.float32)

            @pl.when(l > 0)
            def _():
                h_copy(layer).wait_recv()
                zpad[0:8, :] = halo[layer, 1]

            @pl.when(l < line - 1)
            def _():
                h_copy(layer).wait_send()

        def convolve(layer):
            at_c = pl.ds(pl.multiple_of(j * width, width), width)
            rates = [taps[layer, pl.ds(k, 1), at_c] for k in range(taps_count)]
            for i in range(q):
                conv = jnp.zeros((rows, width), jnp.float32)
                for k in range(taps_count):
                    first = 8 - (taps_count - 1) + k + i * rows
                    conv = conv + rates[k] * zpad[first:first + rows, :]
                at = pl.ds(i * rows, rows)
                gated[at, :] = (obuf[at, :].astype(jnp.float32) * conv).astype(jnp.bfloat16)

        def tile_at(jj):
            return pl.ds(pl.multiple_of(jj * rows, rows), rows)

        def p_copy(layer, r, i):
            at = tile_at(flip(j, i))
            return remote(
                part.at[layer, lax.rem(c + r, tp), at, :], rec1.at[layer, r - 1, at, :],
                p_send.at[layer, r, i], p_recv.at[layer, r, i], at_tp(r),
            )

        def out_product(layer):
            for i in range(q - 1, -1, -1):
                at = tile_at(flip(j, i))

                def half(cc, carry):
                    weight = jnp.concatenate([wout[layer, cc * per_half + b] for b in range(per_half)], axis=1)
                    part[layer, cc, at, :] = jnp.dot(
                        gated[at, :], weight, preferred_element_type=jnp.float32
                    ).astype(jnp.bfloat16)
                    return carry

                lax.fori_loop(0, tp, half, 0)
                for r in range(1, tp):
                    p_copy(layer, r, i).start()

        def r_copy(layer, i):
            return remote(snd2.at[layer, i], rec2.at[layer, i], r_send.at[layer, i], r_recv.at[layer, i], at_sp(peer(i)))

        def reduce_start(layer):
            for i in range(q - 1, -1, -1):
                at = tile_at(flip(j, i))
                total = part[layer, c, at, :].astype(jnp.float32)
                for r in range(1, tp):
                    p_copy(layer, r, i).wait()
                    total = total + rec1[layer, r - 1, at, :].astype(jnp.float32)
                if i:
                    snd2[layer, i] = total.astype(jnp.bfloat16)
                    r_copy(layer, i).start()
                else:
                    acc[...] = total

        def s_copy(layer, r):
            return remote(stat.at[layer], stat_in.at[layer, r], s_send.at[layer, r], s_recv.at[layer, r], at_tp(r))

        def finish(layer):
            pre = alpha * src_of(layer)[...].astype(jnp.float32) + acc[...]
            for i in range(1, q):
                r_copy(layer, i).wait()
                pre = pre + rec2[layer, i].astype(jnp.float32)
            acc[...] = pre
            mine = jnp.sum(pre, axis=-1, keepdims=True)
            away = pre - mine * (1.0 / feats)
            spread = jnp.sum(away * away, axis=-1, keepdims=True)
            lane = lax.broadcasted_iota(jnp.int32, (rows, LANES), 1)
            stat[layer] = jnp.where(lane == 0, mine, spread)
            for r in range(1, tp):
                s_copy(layer, r).start()
            sums, spreads = [mine], [spread]
            for r in range(1, tp):
                s_copy(layer, r).wait()
                sums.append(stat_in[layer, r, :, 0:1])
                spreads.append(stat_in[layer, r, :, 1:2])
            mean = sum(sums[1:], sums[0]) * (1.0 / model)
            var = sum(spreads[1:], spreads[0])
            for s in sums:
                off = s * (1.0 / feats) - mean
                var = var + feats * off * off
            scale = lax.rsqrt(var * (1.0 / model) + EPS)
            normed = (acc[...] - mean) * scale
            y = (normed * gain[pl.ds(layer, 1), :] + bias[pl.ds(layer, 1), :]).astype(jnp.bfloat16)
            if layer == layers - 1:
                res[...] = y
            else:
                state[layer] = y

        for k in range(min(2, units)):
            scatter_start(k)
        gather_start(0)
        for k in range(2, units):
            scatter_start(k)

        def ready(k):
            layer, w = divmod(k, 4)
            if w == 0:
                if layer == 0:
                    gather_wait(0)
                    project(0, 0, put_u)
            elif layer == 0:
                if w == 1:
                    project(0, 1, put_z)
                    halo_start(0)
                elif w == 2:
                    project(0, 2, put_o)
                    halo_wait(0)
                    convolve(0)
                else:
                    out_product(0)

        def layer_rest(layer):
            gather_forward(layer)
            gather_wait(layer)
            project(layer, 0, put_u)
            project(layer, 1, put_z)
            halo_start(layer)
            project(layer, 2, put_o)
            halo_wait(layer)
            convolve(layer)
            out_product(layer)
            reduce_start(layer)
            finish(layer)

        steps = line - 1
        for t in range(units + steps):
            if t < units:
                scatter_wait(t)
                line_start(t, 0)
            for s in range(1, steps):
                if 0 <= t - s < units:
                    line_recv(t - s, s - 1)
                    line_start(t - s, s)
            if t == 1:
                gather_forward(0)
            k = t - steps
            if 0 <= k < units:
                line_recv(k, steps - 1)
                ready(k)
                if k == 4:
                    reduce_start(0)
                if k == 5:
                    finish(0)
                    if layers > 1:
                        gather_start(1)
        for layer in range(1, layers):
            if layer > 1:
                gather_start(layer)
            layer_rest(layer)
        for k in range(units):
            for s in range(steps):
                line_sent(k, s)

    return kernel


def solution(mesh):
    sp, tp = mesh.shape["sp"], mesh.shape["tp"]

    def shards(tokens, value_weight, outer_weight, inner_weight, conv_taps, output_weight, norm_gain, norm_bias):
        rows, feats = tokens.shape
        layers, depth, channels = value_weight.shape
        taps_count = conv_taps.shape[1]
        q = plane_size(sp, channels)
        width = channels // q
        line = sp // q
        model = feats * tp
        alpha = (2.0 * layers) ** 0.25
        out_cols = output_weight.shape[2]
        bf, f32 = jnp.bfloat16, jnp.float32
        kernel = make_kernel(sp, tp, q, layers, taps_count, rows, feats, depth, width, alpha)
        dma = pltpu.SemaphoreType.DMA
        units, steps = 4 * layers, max(line - 1, 1)
        others = max(tp - 1, 1)
        vm = pl.BlockSpec(memory_space=pltpu.VMEM)
        return pl.pallas_call(
            kernel,
            out_shape=jax.ShapeDtypeStruct((rows, feats), bf),
            in_specs=[vm] * 8,
            out_specs=vm,
            scratch_shapes=[
                pltpu.VMEM((layers, tp, q * rows, feats), bf),
                pltpu.VMEM((layers, 3, model, width), bf),
                pltpu.VMEM((layers, sp, width, out_cols), bf),
                pltpu.VMEM((layers, rows, feats), bf),
                pltpu.VMEM((q * rows, width), bf),
                pltpu.VMEM((q * rows, width), bf),
                pltpu.VMEM((q * rows + 8, width), f32),
                pltpu.VMEM((q * rows, width), bf),
                pltpu.VMEM((layers, tp, q * rows, feats), bf),
                pltpu.VMEM((layers, others, q * rows, feats), bf),
                pltpu.VMEM((layers, q, rows, feats), bf),
                pltpu.VMEM((layers, q, rows, feats), bf),
                pltpu.VMEM((rows, feats), f32),
                pltpu.VMEM((layers, rows, LANES), f32),
                pltpu.VMEM((layers, tp, rows, LANES), f32),
                pltpu.VMEM((layers, 2, 8, width), f32),
                dma((units, q)), dma((units, q)), dma((units,)),
                dma((units, steps)), dma((units, steps)), dma((units, steps)), dma((units, steps)),
                dma((layers, q)), dma((layers, q)), dma((layers,)),
                dma((layers, tp, q)), dma((layers, tp, q)),
                dma((layers, tp, q)), dma((layers, tp, q)),
                dma((layers, q)), dma((layers, q)),
                dma((layers, tp)), dma((layers, tp)),
                dma((layers,)), dma((layers,)),
            ],
            compiler_params=pltpu.CompilerParams(
                collective_id=0, has_side_effects=True, vmem_limit_bytes=60 * 1024 * 1024
            ),
        )(tokens, value_weight, outer_weight, inner_weight, conv_taps, output_weight, norm_gain, norm_bias)

    in_specs = (
        P("sp", "tp"),
        P(None, "sp", "tp"),
        P(None, "sp", "tp"),
        P(None, "sp", "tp"),
        P(None, None, "tp"),
        P(None, "tp", "sp"),
        P(None, "tp"),
        P(None, "tp"),
    )
    return jax.shard_map(shards, mesh=mesh, in_specs=in_specs, out_specs=P("sp", "tp"), check_vma=False)
```

```python
import jax
import jax.numpy as jnp
from jax import lax
from jax.experimental import pallas as pl
from jax.experimental.pallas import tpu as pltpu
from jax.sharding import PartitionSpec as P

LANES = 128
EPS = 1e-5


def flip(j, i):
    if i & 1:
        j = j + 1 - 2 * lax.rem(j, 2)
    if i & 2:
        j = j + 2 - 4 * lax.rem(lax.div(j, 2), 2)
    return j


def plane_size(sp, channels):
    q = 4
    while q > 1 and (sp % q or channels // q < LANES or channels % q):
        q //= 2
    return q


def make_kernel(sp, tp, q, layers, taps_count, rows, feats, depth, width, alpha):
    line = sp // q
    units = layers * 4
    model = feats * tp
    per_half = sp // tp

    def kernel(
        tok, val, outw, inn, taps, prj, gain, bias, res,
        xg, win, wout, state, ubuf, obuf, zpad, gated, part, rec1, snd2, rec2, acc, stat, stat_in, halo,
        a_send, a_recv, a_loc, u_send, u_recv, d_send, d_recv,
        g_send, g_recv, g_loc, t_send, t_recv, p_send, p_recv, r_send, r_recv, s_send, s_recv, h_send, h_recv,
    ):
        me = lax.axis_index("sp")
        c = lax.axis_index("tp")
        l = lax.div(me, q)
        j = lax.rem(me, q)

        def at_sp(other):
            return {"sp": other, "tp": c}

        def at_tp(r):
            return {"sp": me, "tp": lax.rem(c + r, tp)}

        def remote(src, dst, ssem, rsem, dev):
            return pltpu.make_async_remote_copy(
                src_ref=src, dst_ref=dst, send_sem=ssem, recv_sem=rsem,
                device_id=dev, device_id_type=pl.DeviceIdType.MESH,
            )

        def peer(i):
            return l * q + flip(j, i)

        barrier = pltpu.get_barrier_semaphore()

        def greet(dev):
            pl.semaphore_signal(barrier, inc=1, device_id=dev, device_id_type=pl.DeviceIdType.MESH)

        for i in range(1, q):
            greet(at_sp(peer(i)))
        for r in range(1, tp):
            greet(at_tp(r))

        @pl.when(l > 0)
        def _():
            greet(at_sp(me - q))

        @pl.when(l < line - 1)
        def _():
            greet(at_sp(me + q))

        neighbours = (l > 0).astype(jnp.int32) + (l < line - 1).astype(jnp.int32)
        pl.semaphore_wait(barrier, (q - 1) + (tp - 1) + neighbours)

        ORDER = (val, inn, outw, prj)

        def own_piece(k, jd):
            layer, w = divmod(k, 4)
            at = pl.ds(pl.multiple_of(jd * width, width), width)
            if w == 3:
                return prj.at[layer, at, :]
            return ORDER[w].at[layer, :, at]

        def landed(k, s):
            layer, w = divmod(k, 4)
            if w == 3:
                return wout.at[layer, s]
            return win.at[layer, w, pl.ds(pl.multiple_of(s * depth, depth), depth), :]

        def block(k, b):
            layer, w = divmod(k, 4)
            if w == 3:
                return wout.at[layer, pl.ds(b * q, q)]
            return win.at[layer, w, pl.ds(pl.multiple_of(b * (q * depth), q * depth), q * depth), :]

        def a_copy(k, i):
            return remote(own_piece(k, flip(j, i)), landed(k, me), a_send.at[k, i], a_recv.at[k, i], at_sp(peer(i)))

        def a_local(k):
            return pltpu.make_async_copy(own_piece(k, j), landed(k, me), a_loc.at[k])

        def scatter_start(k):
            a_local(k).start()
            for i in range(q - 1, 0, -1):
                a_copy(k, i).start()

        def scatter_wait(k):
            a_local(k).wait()
            for i in range(q - 1, 0, -1):
                a_copy(k, i).wait()

        def up(k, s):
            return remote(block(k, l - s), block(k, l - s), u_send.at[k, s], u_recv.at[k, s], at_sp(me + q))

        def down(k, s):
            return remote(block(k, l + s), block(k, l + s), d_send.at[k, s], d_recv.at[k, s], at_sp(me - q))

        def line_start(k, s):
            @pl.when((l - s >= 0) & (l < line - 1))
            def _():
                up(k, s).start()

            @pl.when((l + s < line) & (l > 0))
            def _():
                down(k, s).start()

        def line_recv(k, s):
            @pl.when(l - 1 - s >= 0)
            def _():
                up(k, s).wait_recv()

            @pl.when(l + 1 + s < line)
            def _():
                down(k, s).wait_recv()

        def line_sent(k, s):
            @pl.when((l - s >= 0) & (l < line - 1))
            def _():
                up(k, s).wait_send()

            @pl.when((l + s < line) & (l > 0))
            def _():
                down(k, s).wait_send()

        def src_of(layer):
            return tok if layer == 0 else state.at[layer - 1]

        def spot(layer, jj):
            return xg.at[layer, c, pl.ds(pl.multiple_of(jj * rows, rows), rows), :]

        def g_copy(layer, i):
            return remote(src_of(layer), spot(layer, j), g_send.at[layer, i], g_recv.at[layer, i], at_sp(peer(i)))

        def g_local(layer):
            return pltpu.make_async_copy(src_of(layer), spot(layer, j), g_loc.at[layer])

        def t_copy(layer, r, i):
            jj = flip(j, i)
            src = src_of(layer) if i == 0 else spot(layer, jj)
            return remote(src, spot(layer, jj), t_send.at[layer, r, i], t_recv.at[layer, r, i], at_tp(r))

        def gather_start(layer):
            g_local(layer).start()
            for i in range(q - 1, 0, -1):
                g_copy(layer, i).start()
            for r in range(1, tp):
                t_copy(layer, r, 0).start()

        def gather_forward(layer):
            for i in range(1, q):
                g_copy(layer, i).wait()
                for r in range(1, tp):
                    t_copy(layer, r, i).start()

        def gather_wait(layer):
            g_local(layer).wait()
            for i in range(q):
                for r in range(1, tp):
                    t_copy(layer, r, i).wait()

        def project(layer, w, store):
            def tile(i, carry):
                at = pl.ds(pl.multiple_of(i * rows, rows), rows)
                total = jnp.zeros((rows, width), jnp.float32)
                for cc in range(tp):
                    total = total + jnp.dot(
                        xg[layer, cc, at, :],
                        win[layer, w, pl.ds(cc * feats, feats), :],
                        preferred_element_type=jnp.float32,
                    )
                store(i, total.astype(jnp.bfloat16))
                return carry

            lax.fori_loop(0, q, tile, 0)

        def put_u(i, v):
            ubuf[pl.ds(pl.multiple_of(i * rows, rows), rows), :] = v

        def put_o(i, v):
            obuf[pl.ds(pl.multiple_of(i * rows, rows), rows), :] = v

        def put_z(i, v):
            at = pl.ds(pl.multiple_of(i * rows, rows), rows)
            zpad[pl.ds(pl.multiple_of(8 + i * rows, 8), rows), :] = v.astype(jnp.float32) * ubuf[at, :].astype(jnp.float32)

        def h_copy(layer):
            return remote(
                halo.at[layer, 0], halo.at[layer, 1], h_send.at[layer], h_recv.at[layer], at_sp(me + q)
            )

        def halo_start(layer):
            halo[layer, 0] = zpad[pl.ds(q * rows, 8), :]

            @pl.when(l < line - 1)
            def _():
                h_copy(layer).start()

        def halo_wait(layer):
            zpad[0:8, :] = jnp.zeros((8, width), jnp.float32)

            @pl.when(l > 0)
            def _():
                h_copy(layer).wait_recv()
                zpad[0:8, :] = halo[layer, 1]

            @pl.when(l < line - 1)
            def _():
                h_copy(layer).wait_send()

        def convolve(layer):
            at_c = pl.ds(pl.multiple_of(j * width, width), width)
            rates = [taps[layer, pl.ds(k, 1), at_c] for k in range(taps_count)]
            for i in range(q):
                conv = jnp.zeros((rows, width), jnp.float32)
                for k in range(taps_count):
                    first = 8 - (taps_count - 1) + k + i * rows
                    conv = conv + rates[k] * zpad[first:first + rows, :]
                at = pl.ds(i * rows, rows)
                gated[at, :] = (obuf[at, :].astype(jnp.float32) * conv).astype(jnp.bfloat16)

        def tile_at(jj):
            return pl.ds(pl.multiple_of(jj * rows, rows), rows)

        def p_copy(layer, r, i):
            at = tile_at(flip(j, i))
            return remote(
                part.at[layer, lax.rem(c + r, tp), at, :], rec1.at[layer, r - 1, at, :],
                p_send.at[layer, r, i], p_recv.at[layer, r, i], at_tp(r),
            )

        def r_copy(layer, i):
            return remote(snd2.at[layer, i], rec2.at[layer, i], r_send.at[layer, i], r_recv.at[layer, i], at_sp(peer(i)))

        def reduce_tile(layer, i):
            at = tile_at(flip(j, i))
            total = part[layer, c, at, :].astype(jnp.float32)
            for r in range(1, tp):
                p_copy(layer, r, i).wait()
                total = total + rec1[layer, r - 1, at, :].astype(jnp.float32)
            if i:
                snd2[layer, i] = total.astype(jnp.bfloat16)
                r_copy(layer, i).start()
            else:
                acc[...] = total

        def out_product(layer):
            for i in range(q - 1, -1, -1):
                at = tile_at(flip(j, i))

                def half(n, carry):
                    cc = lax.rem(c + 1 + n, tp)
                    weight = jnp.concatenate([wout[layer, cc * per_half + b] for b in range(per_half)], axis=1)
                    part[layer, cc, at, :] = jnp.dot(
                        gated[at, :], weight, preferred_element_type=jnp.float32
                    ).astype(jnp.bfloat16)
                    return carry

                lax.fori_loop(0, tp, half, 0)
                for r in range(1, tp):
                    p_copy(layer, r, i).start()
                if i < q - 1:
                    reduce_tile(layer, i + 1)
            reduce_tile(layer, 0)

        def s_copy(layer, r):
            return remote(stat.at[layer], stat_in.at[layer, r], s_send.at[layer, r], s_recv.at[layer, r], at_tp(r))

        def finish(layer):
            pre = alpha * src_of(layer)[...].astype(jnp.float32) + acc[...]
            for i in range(1, q):
                r_copy(layer, i).wait()
                pre = pre + rec2[layer, i].astype(jnp.float32)
            acc[...] = pre
            mine = jnp.sum(pre, axis=-1, keepdims=True)
            away = pre - mine * (1.0 / feats)
            spread = jnp.sum(away * away, axis=-1, keepdims=True)
            lane = lax.broadcasted_iota(jnp.int32, (rows, LANES), 1)
            stat[layer] = jnp.where(lane == 0, mine, spread)
            for r in range(1, tp):
                s_copy(layer, r).start()
            sums, spreads = [mine], [spread]
            for r in range(1, tp):
                s_copy(layer, r).wait()
                sums.append(stat_in[layer, r, :, 0:1])
                spreads.append(stat_in[layer, r, :, 1:2])
            mean = sum(sums[1:], sums[0]) * (1.0 / model)
            var = sum(spreads[1:], spreads[0])
            for s in sums:
                off = s * (1.0 / feats) - mean
                var = var + feats * off * off
            scale = lax.rsqrt(var * (1.0 / model) + EPS)
            normed = (acc[...] - mean) * scale
            y = (normed * gain[pl.ds(layer, 1), :] + bias[pl.ds(layer, 1), :]).astype(jnp.bfloat16)
            if layer == layers - 1:
                res[...] = y
            else:
                state[layer] = y

        for k in range(min(2, units)):
            scatter_start(k)
        gather_start(0)
        for k in range(2, units):
            scatter_start(k)

        def inputs_of(layer):
            gather_wait(layer)
            project(layer, 0, put_u)

        def middle_of(layer):
            project(layer, 1, put_z)
            halo_start(layer)

        def gates_of(layer):
            project(layer, 2, put_o)
            halo_wait(layer)
            convolve(layer)

        steps = line - 1
        begin = [k + k // 4 for k in range(units)]
        for t in range(begin[-1] + steps + 1):
            for k in range(units):
                if begin[k] == t:
                    scatter_wait(k)
                    line_start(k, 0)
            for k in range(units):
                s = t - begin[k]
                if 1 <= s < steps:
                    line_recv(k, s - 1)
                    line_start(k, s)
            for k in range(units):
                if t - begin[k] == steps:
                    line_recv(k, steps - 1)
            if t == begin[0] + steps - 1:
                gather_forward(0)
            if t == begin[0] + steps:
                inputs_of(0)
            if t == begin[1] + steps:
                middle_of(0)
            if t == begin[2] + steps:
                gates_of(0)
            if t == begin[3] + steps:
                out_product(0)
            if layers > 1:
                if t == begin[3] + steps + 1:
                    finish(0)
                    gather_start(1)
                if t == begin[3] + steps + 3:
                    gather_forward(1)
                if t == begin[3] + steps + 4:
                    inputs_of(1)
                    middle_of(1)
                    gates_of(1)
        if layers > 1:
            out_product(1)
            finish(1)
        for layer in range(2, layers):
            gather_start(layer)
            gather_forward(layer)
            inputs_of(layer)
            middle_of(layer)
            gates_of(layer)
            out_product(layer)
            finish(layer)
        for k in range(units):
            for s in range(steps):
                line_sent(k, s)

    return kernel


def solution(mesh):
    sp, tp = mesh.shape["sp"], mesh.shape["tp"]

    def shards(tokens, value_weight, outer_weight, inner_weight, conv_taps, output_weight, norm_gain, norm_bias):
        rows, feats = tokens.shape
        layers, depth, channels = value_weight.shape
        taps_count = conv_taps.shape[1]
        q = plane_size(sp, channels)
        width = channels // q
        line = sp // q
        model = feats * tp
        alpha = (2.0 * layers) ** 0.25
        out_cols = output_weight.shape[2]
        bf, f32 = jnp.bfloat16, jnp.float32
        kernel = make_kernel(sp, tp, q, layers, taps_count, rows, feats, depth, width, alpha)
        dma = pltpu.SemaphoreType.DMA
        units, steps = 4 * layers, max(line - 1, 1)
        others = max(tp - 1, 1)
        vm = pl.BlockSpec(memory_space=pltpu.VMEM)
        return pl.pallas_call(
            kernel,
            out_shape=jax.ShapeDtypeStruct((rows, feats), bf),
            in_specs=[vm] * 8,
            out_specs=vm,
            scratch_shapes=[
                pltpu.VMEM((layers, tp, q * rows, feats), bf),
                pltpu.VMEM((layers, 3, model, width), bf),
                pltpu.VMEM((layers, sp, width, out_cols), bf),
                pltpu.VMEM((layers, rows, feats), bf),
                pltpu.VMEM((q * rows, width), bf),
                pltpu.VMEM((q * rows, width), bf),
                pltpu.VMEM((q * rows + 8, width), f32),
                pltpu.VMEM((q * rows, width), bf),
                pltpu.VMEM((layers, tp, q * rows, feats), bf),
                pltpu.VMEM((layers, others, q * rows, feats), bf),
                pltpu.VMEM((layers, q, rows, feats), bf),
                pltpu.VMEM((layers, q, rows, feats), bf),
                pltpu.VMEM((rows, feats), f32),
                pltpu.VMEM((layers, rows, LANES), f32),
                pltpu.VMEM((layers, tp, rows, LANES), f32),
                pltpu.VMEM((layers, 2, 8, width), f32),
                dma((units, q)), dma((units, q)), dma((units,)),
                dma((units, steps)), dma((units, steps)), dma((units, steps)), dma((units, steps)),
                dma((layers, q)), dma((layers, q)), dma((layers,)),
                dma((layers, tp, q)), dma((layers, tp, q)),
                dma((layers, tp, q)), dma((layers, tp, q)),
                dma((layers, q)), dma((layers, q)),
                dma((layers, tp)), dma((layers, tp)),
                dma((layers,)), dma((layers,)),
            ],
            compiler_params=pltpu.CompilerParams(
                collective_id=0, has_side_effects=True, vmem_limit_bytes=60 * 1024 * 1024
            ),
        )(tokens, value_weight, outer_weight, inner_weight, conv_taps, output_weight, norm_gain, norm_bias)

    in_specs = (
        P("sp", "tp"),
        P(None, "sp", "tp"),
        P(None, "sp", "tp"),
        P(None, "sp", "tp"),
        P(None, None, "tp"),
        P(None, "tp", "sp"),
        P(None, "tp"),
        P(None, "tp"),
    )
    return jax.shard_map(shards, mesh=mesh, in_specs=in_specs, out_specs=P("sp", "tp"), check_vma=False)
```

```python
import jax
import jax.numpy as jnp
from jax import lax
from jax.experimental import pallas as pl
from jax.experimental.pallas import tpu as pltpu
from jax.sharding import PartitionSpec as P

LANES = 128
EPS = 1e-5


def flip(j, i):
    if i & 1:
        j = j + 1 - 2 * lax.rem(j, 2)
    if i & 2:
        j = j + 2 - 4 * lax.rem(lax.div(j, 2), 2)
    return j


def plane_size(sp, channels):
    q = 4
    while q > 1 and (sp % q or channels // q < LANES or channels % q):
        q //= 2
    return q


def make_kernel(sp, tp, q, layers, taps_count, rows, feats, depth, width, alpha):
    line = sp // q
    units = layers * 4
    model = feats * tp
    per_half = sp // tp

    def kernel(
        tok, val, outw, inn, taps, prj, gain, bias, res,
        xg, win, wout, state, ubuf, obuf, zpad, gated, part, rec1, snd2, rec2, acc, stat, stat_in, halo,
        a_send, a_recv, a_loc, u_send, u_recv, d_send, d_recv,
        g_send, g_recv, g_loc, t_send, t_recv, p_send, p_recv, r_send, r_recv, s_send, s_recv, h_send, h_recv,
    ):
        me = lax.axis_index("sp")
        c = lax.axis_index("tp")
        l = lax.div(me, q)
        j = lax.rem(me, q)

        def at_sp(other):
            return {"sp": other, "tp": c}

        def at_tp(r):
            return {"sp": me, "tp": lax.rem(c + r, tp)}

        def remote(src, dst, ssem, rsem, dev):
            return pltpu.make_async_remote_copy(
                src_ref=src, dst_ref=dst, send_sem=ssem, recv_sem=rsem,
                device_id=dev, device_id_type=pl.DeviceIdType.MESH,
            )

        def peer(i):
            return l * q + flip(j, i)

        barrier = pltpu.get_barrier_semaphore()

        def greet(dev):
            pl.semaphore_signal(barrier, inc=1, device_id=dev, device_id_type=pl.DeviceIdType.MESH)

        for i in range(1, q):
            greet(at_sp(peer(i)))
        for r in range(1, tp):
            greet(at_tp(r))

        @pl.when(l > 0)
        def _():
            greet(at_sp(me - q))

        @pl.when(l < line - 1)
        def _():
            greet(at_sp(me + q))

        neighbours = (l > 0).astype(jnp.int32) + (l < line - 1).astype(jnp.int32)
        pl.semaphore_wait(barrier, (q - 1) + (tp - 1) + neighbours)

        ORDER = (val, inn, outw, prj)

        def own_piece(k, jd):
            layer, w = divmod(k, 4)
            at = pl.ds(pl.multiple_of(jd * width, width), width)
            if w == 3:
                return prj.at[layer, at, :]
            return ORDER[w].at[layer, :, at]

        def landed(k, s):
            layer, w = divmod(k, 4)
            if w == 3:
                return wout.at[layer, s]
            return win.at[layer, w, pl.ds(pl.multiple_of(s * depth, depth), depth), :]

        def block(k, b):
            layer, w = divmod(k, 4)
            if w == 3:
                return wout.at[layer, pl.ds(b * q, q)]
            return win.at[layer, w, pl.ds(pl.multiple_of(b * (q * depth), q * depth), q * depth), :]

        def a_copy(k, i):
            return remote(own_piece(k, flip(j, i)), landed(k, me), a_send.at[k, i], a_recv.at[k, i], at_sp(peer(i)))

        def a_local(k):
            return pltpu.make_async_copy(own_piece(k, j), landed(k, me), a_loc.at[k])

        def scatter_start(k):
            a_local(k).start()
            for i in range(q - 1, 0, -1):
                a_copy(k, i).start()

        def scatter_wait(k):
            a_local(k).wait()
            for i in range(q - 1, 0, -1):
                a_copy(k, i).wait()

        def up(k, s):
            return remote(block(k, l - s), block(k, l - s), u_send.at[k, s], u_recv.at[k, s], at_sp(me + q))

        def down(k, s):
            return remote(block(k, l + s), block(k, l + s), d_send.at[k, s], d_recv.at[k, s], at_sp(me - q))

        def line_start(k, s):
            @pl.when((l - s >= 0) & (l < line - 1))
            def _():
                up(k, s).start()

            @pl.when((l + s < line) & (l > 0))
            def _():
                down(k, s).start()

        def line_recv(k, s):
            @pl.when(l - 1 - s >= 0)
            def _():
                up(k, s).wait_recv()

            @pl.when(l + 1 + s < line)
            def _():
                down(k, s).wait_recv()

        def line_sent(k, s):
            @pl.when((l - s >= 0) & (l < line - 1))
            def _():
                up(k, s).wait_send()

            @pl.when((l + s < line) & (l > 0))
            def _():
                down(k, s).wait_send()

        def src_of(layer):
            return tok if layer == 0 else state.at[layer - 1]

        def spot(layer, jj):
            return xg.at[layer, c, pl.ds(pl.multiple_of(jj * rows, rows), rows), :]

        def g_copy(layer, i):
            return remote(src_of(layer), spot(layer, j), g_send.at[layer, i], g_recv.at[layer, i], at_sp(peer(i)))

        def g_local(layer):
            return pltpu.make_async_copy(src_of(layer), spot(layer, j), g_loc.at[layer])

        def t_copy(layer, r, i):
            jj = flip(j, i)
            src = src_of(layer) if i == 0 else spot(layer, jj)
            return remote(src, spot(layer, jj), t_send.at[layer, r, i], t_recv.at[layer, r, i], at_tp(r))

        def gather_start(layer):
            g_local(layer).start()
            for i in range(q - 1, 0, -1):
                g_copy(layer, i).start()
            for r in range(1, tp):
                t_copy(layer, r, 0).start()

        def gather_forward(layer):
            for i in range(1, q):
                g_copy(layer, i).wait()
                for r in range(1, tp):
                    t_copy(layer, r, i).start()

        def gather_wait(layer):
            g_local(layer).wait()
            for i in range(q):
                for r in range(1, tp):
                    t_copy(layer, r, i).wait()

        def project(layer, w, store):
            def tile(i, carry):
                at = pl.ds(pl.multiple_of(i * rows, rows), rows)
                total = jnp.zeros((rows, width), jnp.float32)
                for cc in range(tp):
                    total = total + jnp.dot(
                        xg[layer, cc, at, :],
                        win[layer, w, pl.ds(cc * feats, feats), :],
                        preferred_element_type=jnp.float32,
                    )
                store(i, total.astype(jnp.bfloat16))
                return carry

            lax.fori_loop(0, q, tile, 0)

        def put_u(i, v):
            ubuf[pl.ds(pl.multiple_of(i * rows, rows), rows), :] = v

        def put_o(i, v):
            obuf[pl.ds(pl.multiple_of(i * rows, rows), rows), :] = v

        def put_z(i, v):
            at = pl.ds(pl.multiple_of(i * rows, rows), rows)
            zpad[pl.ds(pl.multiple_of(8 + i * rows, 8), rows), :] = v.astype(jnp.float32) * ubuf[at, :].astype(jnp.float32)

        def h_copy(layer):
            return remote(
                halo.at[layer, 0], halo.at[layer, 1], h_send.at[layer], h_recv.at[layer], at_sp(me + q)
            )

        def halo_start(layer):
            halo[layer, 0] = zpad[pl.ds(q * rows, 8), :]

            @pl.when(l < line - 1)
            def _():
                h_copy(layer).start()

        def halo_wait(layer):
            zpad[0:8, :] = jnp.zeros((8, width), jnp.float32)

            @pl.when(l > 0)
            def _():
                h_copy(layer).wait_recv()
                zpad[0:8, :] = halo[layer, 1]

            @pl.when(l < line - 1)
            def _():
                h_copy(layer).wait_send()

        def convolve(layer):
            at_c = pl.ds(pl.multiple_of(j * width, width), width)
            rates = [taps[layer, pl.ds(k, 1), at_c] for k in range(taps_count)]
            for i in range(q):
                conv = jnp.zeros((rows, width), jnp.float32)
                for k in range(taps_count):
                    first = 8 - (taps_count - 1) + k + i * rows
                    conv = conv + rates[k] * zpad[first:first + rows, :]
                at = pl.ds(i * rows, rows)
                gated[at, :] = (obuf[at, :].astype(jnp.float32) * conv).astype(jnp.bfloat16)

        def tile_at(jj):
            return pl.ds(pl.multiple_of(jj * rows, rows), rows)

        def p_copy(layer, r, i):
            at = tile_at(flip(j, i))
            return remote(
                part.at[layer, lax.rem(c + r, tp), at, :], rec1.at[layer, r - 1, at, :],
                p_send.at[layer, r, i], p_recv.at[layer, r, i], at_tp(r),
            )

        halves = 2 if q == 4 else 1
        part_rows = rows // halves

        def rows_of(h):
            return pl.ds(h * part_rows, part_rows)

        def r_copy(layer, i, h):
            at = rows_of(h)
            return remote(
                snd2.at[layer, i, at, :], rec2.at[layer, i, at, :],
                r_send.at[layer, i, h], r_recv.at[layer, i, h], at_sp(peer(i)),
            )

        def v_copy(layer, h):
            at = rows_of(h)
            return remote(
                snd2.at[layer, 3, at, :], rec2.at[layer, 3, at, :],
                r_send.at[layer, 3, h], r_recv.at[layer, 3, h], at_sp(peer(1 + h)),
            )

        def reduce_tile(layer, i):
            at = tile_at(flip(j, i))
            total = part[layer, c, at, :].astype(jnp.float32)
            for r in range(1, tp):
                p_copy(layer, r, i).wait()
                total = total + rec1[layer, r - 1, at, :].astype(jnp.float32)
            if i == 0:
                acc[...] = total
                return
            snd2[layer, i] = total.astype(jnp.bfloat16)
            if i == 3:
                for h in range(2):
                    v_copy(layer, h).start()
            elif halves == 2:
                r_copy(layer, i, i - 1).start()
            else:
                r_copy(layer, i, 0).start()

        def relay(layer):
            if halves == 2:
                for h in range(2):
                    v_copy(layer, h).wait()
                    i, at = 2 - h, rows_of(h)
                    snd2[layer, i, at, :] = (
                        snd2[layer, i, at, :].astype(jnp.float32) + rec2[layer, 3, at, :].astype(jnp.float32)
                    ).astype(jnp.bfloat16)
                    r_copy(layer, i, h).start()

        def out_product(layer):
            for i in range(q - 1, -1, -1):
                at = tile_at(flip(j, i))

                def half(n, carry):
                    cc = lax.rem(c + 1 + n, tp)
                    weight = jnp.concatenate([wout[layer, cc * per_half + b] for b in range(per_half)], axis=1)
                    part[layer, cc, at, :] = jnp.dot(
                        gated[at, :], weight, preferred_element_type=jnp.float32
                    ).astype(jnp.bfloat16)
                    return carry

                lax.fori_loop(0, tp, half, 0)
                for r in range(1, tp):
                    p_copy(layer, r, i).start()
                if i < q - 1:
                    reduce_tile(layer, i + 1)
            reduce_tile(layer, 0)
            relay(layer)

        def s_copy(layer, r):
            return remote(stat.at[layer], stat_in.at[layer, r], s_send.at[layer, r], s_recv.at[layer, r], at_tp(r))

        def finish(layer):
            pre = alpha * src_of(layer)[...].astype(jnp.float32) + acc[...]
            for i in range(1, min(q, 3)):
                for h in range(halves):
                    r_copy(layer, i, h).wait()
                pre = pre + rec2[layer, i].astype(jnp.float32)
            acc[...] = pre
            mine = jnp.sum(pre, axis=-1, keepdims=True)
            away = pre - mine * (1.0 / feats)
            spread = jnp.sum(away * away, axis=-1, keepdims=True)
            lane = lax.broadcasted_iota(jnp.int32, (rows, LANES), 1)
            stat[layer] = jnp.where(lane == 0, mine, spread)
            for r in range(1, tp):
                s_copy(layer, r).start()
            sums, spreads = [mine], [spread]
            for r in range(1, tp):
                s_copy(layer, r).wait()
                sums.append(stat_in[layer, r, :, 0:1])
                spreads.append(stat_in[layer, r, :, 1:2])
            mean = sum(sums[1:], sums[0]) * (1.0 / model)
            var = sum(spreads[1:], spreads[0])
            for s in sums:
                off = s * (1.0 / feats) - mean
                var = var + feats * off * off
            scale = lax.rsqrt(var * (1.0 / model) + EPS)
            normed = (acc[...] - mean) * scale
            y = (normed * gain[pl.ds(layer, 1), :] + bias[pl.ds(layer, 1), :]).astype(jnp.bfloat16)
            if layer == layers - 1:
                res[...] = y
            else:
                state[layer] = y

        for k in range(min(2, units)):
            scatter_start(k)
        gather_start(0)
        for k in range(2, units):
            scatter_start(k)

        def inputs_of(layer):
            gather_wait(layer)
            project(layer, 0, put_u)

        def middle_of(layer):
            project(layer, 1, put_z)
            halo_start(layer)

        def gates_of(layer):
            project(layer, 2, put_o)
            halo_wait(layer)
            convolve(layer)

        steps = line - 1
        begin = [k + k // 4 for k in range(units)]
        for t in range(begin[-1] + steps + 1):
            for k in range(units):
                if begin[k] == t:
                    scatter_wait(k)
                    line_start(k, 0)
            for k in range(units):
                s = t - begin[k]
                if 1 <= s < steps:
                    line_recv(k, s - 1)
                    line_start(k, s)
            for k in range(units):
                if t - begin[k] == steps:
                    line_recv(k, steps - 1)
            if t == begin[0] + steps - 1:
                gather_forward(0)
            if t == begin[0] + steps:
                inputs_of(0)
            if t == begin[1] + steps:
                middle_of(0)
            if t == begin[2] + steps:
                gates_of(0)
            if t == begin[3] + steps:
                out_product(0)
            if layers > 1:
                if t == begin[3] + steps + 1:
                    finish(0)
                    gather_start(1)
                if t == begin[3] + steps + 3:
                    gather_forward(1)
                if t == begin[3] + steps + 4:
                    inputs_of(1)
                    middle_of(1)
                    gates_of(1)
        if layers > 1:
            out_product(1)
            finish(1)
        for layer in range(2, layers):
            gather_start(layer)
            gather_forward(layer)
            inputs_of(layer)
            middle_of(layer)
            gates_of(layer)
            out_product(layer)
            finish(layer)
        for k in range(units):
            for s in range(steps):
                line_sent(k, s)

    return kernel


def solution(mesh):
    sp, tp = mesh.shape["sp"], mesh.shape["tp"]

    def shards(tokens, value_weight, outer_weight, inner_weight, conv_taps, output_weight, norm_gain, norm_bias):
        rows, feats = tokens.shape
        layers, depth, channels = value_weight.shape
        taps_count = conv_taps.shape[1]
        q = plane_size(sp, channels)
        width = channels // q
        line = sp // q
        model = feats * tp
        alpha = (2.0 * layers) ** 0.25
        out_cols = output_weight.shape[2]
        bf, f32 = jnp.bfloat16, jnp.float32
        kernel = make_kernel(sp, tp, q, layers, taps_count, rows, feats, depth, width, alpha)
        dma = pltpu.SemaphoreType.DMA
        units, steps = 4 * layers, max(line - 1, 1)
        others = max(tp - 1, 1)
        vm = pl.BlockSpec(memory_space=pltpu.VMEM)
        return pl.pallas_call(
            kernel,
            out_shape=jax.ShapeDtypeStruct((rows, feats), bf),
            in_specs=[vm] * 8,
            out_specs=vm,
            scratch_shapes=[
                pltpu.VMEM((layers, tp, q * rows, feats), bf),
                pltpu.VMEM((layers, 3, model, width), bf),
                pltpu.VMEM((layers, sp, width, out_cols), bf),
                pltpu.VMEM((layers, rows, feats), bf),
                pltpu.VMEM((q * rows, width), bf),
                pltpu.VMEM((q * rows, width), bf),
                pltpu.VMEM((q * rows + 8, width), f32),
                pltpu.VMEM((q * rows, width), bf),
                pltpu.VMEM((layers, tp, q * rows, feats), bf),
                pltpu.VMEM((layers, others, q * rows, feats), bf),
                pltpu.VMEM((layers, q, rows, feats), bf),
                pltpu.VMEM((layers, q, rows, feats), bf),
                pltpu.VMEM((rows, feats), f32),
                pltpu.VMEM((layers, rows, LANES), f32),
                pltpu.VMEM((layers, tp, rows, LANES), f32),
                pltpu.VMEM((layers, 2, 8, width), f32),
                dma((units, q)), dma((units, q)), dma((units,)),
                dma((units, steps)), dma((units, steps)), dma((units, steps)), dma((units, steps)),
                dma((layers, q)), dma((layers, q)), dma((layers,)),
                dma((layers, tp, q)), dma((layers, tp, q)),
                dma((layers, tp, q)), dma((layers, tp, q)),
                dma((layers, q, 2)), dma((layers, q, 2)),
                dma((layers, tp)), dma((layers, tp)),
                dma((layers,)), dma((layers,)),
            ],
            compiler_params=pltpu.CompilerParams(
                collective_id=0, has_side_effects=True, vmem_limit_bytes=60 * 1024 * 1024
            ),
        )(tokens, value_weight, outer_weight, inner_weight, conv_taps, output_weight, norm_gain, norm_bias)

    in_specs = (
        P("sp", "tp"),
        P(None, "sp", "tp"),
        P(None, "sp", "tp"),
        P(None, "sp", "tp"),
        P(None, None, "tp"),
        P(None, "tp", "sp"),
        P(None, "tp"),
        P(None, "tp"),
    )
    return jax.shard_map(shards, mesh=mesh, in_specs=in_specs, out_specs=P("sp", "tp"), check_vma=False)
```
